512 devices in a mesh: grp: 2 (over y), sp: 16 (over z), tp: 16 (over x, core).
Axes of the slice: x: 8, y: 2, z: 16, core: 2. Of those that a mesh axis runs over, the one named last changes fastest.
The devices are a block of a 8x16x16 slice.
Arguments:
- tokens: bfloat16 [8192, 2048], P(('grp', 'sp'), 'tp'), parts along dimension 0, may hold values from -40 to 40
- norm_gain: float32 [2, 2048], replicated, may hold values from 0.1 to 1.9
- value_proj: bfloat16 [2, 1024, 2048], P(None, 'tp', 'sp'), may hold values from -0.125 to 0.125
- gate_proj: bfloat16 [2, 1024, 2048], P(None, 'tp', 'sp'), may hold values from -0.125 to 0.125
- conv_taps: float32 [2, 4, 1024], P(None, None, 'tp'), may hold values from -3 to 3
- recur_map: bfloat16 [2, 16, 64, 64], P(None, 'tp'), may hold values from -0.75 to 0.75
- input_map: bfloat16 [2, 16, 64, 64], P(None, 'tp'), may hold values from -0.75 to 0.75
- decay_param: float32 [2, 1024], P(None, 'tp'), may hold values from 3 to 16
- decay_offset: float32 [2, 1024, 4096], P(None, 'tp', 'sp'), may hold values from -3 to 0
- mix_proj: bfloat16 [2, 1024, 2048], P(None, 'sp', 'tp'), may hold values from -0.1875 to 0.1875
Outputs:
- mixed_out: bfloat16 [8192, 2048], P(('grp', 'sp'), 'tp'), parts along dimension 0
The draws below stay inside these ranges and needn't reach their ends.
There are 2 independent parts, one for each index of `grp`. The reference program is written for one: setup_inputs(seed, part) draws one part's arguments, and reference() takes and returns one part's arrays. A program takes and returns all parts, laid end to end along the dimension named above; an argument that names none is the same for every part. Nothing has to cross between parts.
All inputs are finite; a program needn't handle non-finite values.
Results may differ from the reference program's by a relative error of at most 0.013.
Values may be sent and summed in bfloat16 or wider, within the bound.
A program may use at most 64 MiB of HBM per device.

```python
import jax
import jax.numpy as jnp
from jax import lax

D = 2048
HEADS = 16
D_LRU = 1024
HEAD_DIM = 64
CONV = 4
LAYERS = 2
TOK_DEV = 256
LENGTH = 4096


def channel_rates(key):
    base = jax.random.fold_in(key, 11)
    keys = jax.random.split(base, 3)
    shape = (LAYERS, D // 2)
    share = 0.5
    fastest = jax.random.uniform(keys[0], shape, jnp.float32) < share
    short_span = min(30, TOK_DEV // 4) * 1.0
    long_span = min(100, TOK_DEV // 2) * 1.0
    fast_span = jnp.exp(jax.random.uniform(keys[1], shape, jnp.float32, jnp.log(short_span), jnp.log(long_span)))
    slow_rate = jnp.exp(jax.random.uniform(keys[2], shape, jnp.float32, jnp.log(0.01), jnp.log(0.04))) / LENGTH
    return jnp.where(fastest, 0.25 / fast_span, slow_rate)


def draw_decay_param(key, part):
    rates = channel_rates(key)
    return -jnp.log(jnp.expm1(rates))


def draw_decay_offset(key, part):
    rates = channel_rates(key)
    keys = jax.random.split(jax.random.fold_in(key, 23), 3)
    blocks = LENGTH // TOK_DEV
    stretch = jnp.exp(jax.random.uniform(keys[0], (LAYERS, D // 2, blocks), jnp.float32, 0.0, jnp.log(3.0)))
    stretch = jnp.repeat(stretch, TOK_DEV, axis=2)
    reference_level = -4.0 * rates[:, :, None] * (stretch - 1.0)
    slot_positions = jax.random.randint(keys[1], (LAYERS, 3), 0, LENGTH)
    share_part = jax.random.uniform(keys[2], (LAYERS, 3, D // 2), jnp.float32, 0.2, 0.5)
    match_count = (slot_positions[:, :, None] == jnp.arange(LENGTH)[None, None, :]).astype(jnp.float32)
    spike_groups = jnp.einsum('rkv,rkq->rvq', jnp.log1p(-share_part), match_count)
    return (reference_level + spike_groups).astype(jnp.float32)


def draw_tokens(key, part):
    keys = jax.random.split(key, 3)
    noise = jnp.clip(jax.random.normal(keys[0], (LENGTH, D), jnp.float32), -4.0, 4.0)
    row_scale = jnp.exp(jax.random.uniform(keys[1], (LENGTH, 1), jnp.float32, 0.0, jnp.log(10.0))) / 5.0
    column_upper = 3.0
    position = jnp.arange(D, dtype=jnp.float32)[None, :] / D
    jitter = jax.random.uniform(keys[2], (1, D), jnp.float32, -0.3, 0.3)
    column_scale = jnp.exp(jnp.log(column_upper) * position + jitter)
    return (noise * row_scale * column_scale).astype(jnp.bfloat16)


def steps_of(own_key, dims, cuts, low, top_value):
    gain = 1.0
    for dim, blocks in cuts:
        steps = jax.random.uniform(jax.random.fold_in(jax.random.fold_in(own_key, 6), dim), (blocks,), jnp.float32, low / len(cuts), top_value / len(cuts))
        gain = gain * jnp.repeat(jnp.exp(steps), dims[dim] // blocks).reshape((-1,) + (1,) * (len(dims) - 1 - dim))
    return gain


def gaussian(stream_key, dims, spread, most, shards=(), held_as=jnp.bfloat16):
    level = steps_of(stream_key, dims, shards, -0.22, 0.18) if shards else 1.0
    result = jax.random.normal(stream_key, dims, jnp.float32) * spread * level
    return jnp.minimum(jnp.maximum(result, -most), most).astype(held_as)


def setup_inputs(seed: int = 0, part: int = 0) -> dict:
    streams_of = jax.random.split(jax.random.key(seed), 11)
    own_keys = jax.random.split(jax.random.fold_in(streams_of[10], part), 11)
    return {
        "tokens": draw_tokens(jax.random.fold_in(jax.random.fold_in(streams_of[10], part), 71), part),
        "norm_gain": jnp.clip(1.0 + 0.18 * jax.random.normal(streams_of[1], (LAYERS, D), jnp.float32), 0.1, 1.9),
        "value_proj": gaussian(streams_of[2], (LAYERS, D_LRU, D), D ** -0.5, 0.125, ((1, 16), (2, 16))),
        "gate_proj": gaussian(streams_of[3], (LAYERS, D_LRU, D), D ** -0.5, 0.125, ((1, 16), (2, 16))),
        "conv_taps": gaussian(streams_of[4], (LAYERS, CONV, D_LRU), CONV ** -0.5, 3.0, ((2, 16),), jnp.float32),
        "recur_map": gaussian(streams_of[5], (LAYERS, HEADS, HEAD_DIM, HEAD_DIM), HEAD_DIM ** -0.5, 0.75, ((1, 16),)),
        "input_map": gaussian(streams_of[6], (LAYERS, HEADS, HEAD_DIM, HEAD_DIM), HEAD_DIM ** -0.5, 0.75, ((1, 16),)),
        "decay_param": draw_decay_param(jax.random.fold_in(streams_of[10], 71), part),
        "decay_offset": draw_decay_offset(jax.random.fold_in(streams_of[10], 71), part),
        "mix_proj": gaussian(streams_of[9], (LAYERS, D_LRU, D), D_LRU ** -0.5, 0.1875, ((1, 16), (2, 16))),
    }


EPS = 1e-06
RATE_SCALE = 8.0

def combine_pairs(earlier, later):
    return (earlier[0] * later[0], later[0] * earlier[1] + later[1])

def mixer_layer(residual, gain_row, value_weights, gate_weights, taps_layer, recur_layer, input_layer, param_layer, offset_layer, mix_weights):
    wide = residual.astype(jnp.float32)
    scale_factor = lax.rsqrt(lax.optimization_barrier(jnp.mean(wide * wide, axis=1)) + EPS)
    scaled = (wide * gain_row[None, :]).astype(jnp.bfloat16)
    value_rows = (jnp.dot(value_weights, scaled.T, preferred_element_type=jnp.float32) * scale_factor[None, :]).astype(jnp.bfloat16)
    gate_rows = (jnp.dot(gate_weights, scaled.T, preferred_element_type=jnp.float32) * scale_factor[None, :]).astype(jnp.bfloat16)
    padded = jnp.concatenate([jnp.zeros((D_LRU, CONV - 1), jnp.bfloat16), value_rows], axis=1)
    smoothed = jnp.zeros((D_LRU, LENGTH), jnp.float32)
    for tap_index in range(CONV):
        smoothed = smoothed + taps_layer[tap_index][:, None] * padded[:, tap_index:tap_index + LENGTH].astype(jnp.float32)
    smoothed_half = smoothed.astype(jnp.bfloat16).astype(jnp.float32).reshape(HEADS, HEAD_DIM, LENGTH)
    recur = jax.nn.sigmoid(jnp.einsum('hit,hij->hjt', smoothed_half, recur_layer.astype(jnp.float32)).reshape(D_LRU, LENGTH))
    inputs = jax.nn.sigmoid(jnp.einsum('hit,hij->hjt', smoothed_half, input_layer.astype(jnp.float32)).reshape(D_LRU, LENGTH))
    log_decay = -RATE_SCALE * recur * jax.nn.softplus(-param_layer)[:, None] + offset_layer
    decay = jnp.exp(log_decay)
    driving = jnp.sqrt(-jnp.expm1(2.0 * log_decay)) * inputs * smoothed
    _, hidden_state = lax.associative_scan(combine_pairs, (decay, driving), axis=1)
    branch = (hidden_state * jax.nn.silu(gate_rows.astype(jnp.float32))).astype(jnp.bfloat16)
    projected = jnp.dot(branch.T, mix_weights, preferred_element_type=jnp.float32)
    return (wide + projected).astype(jnp.bfloat16)

def reference(tokens, norm_gain, value_proj, gate_proj, conv_taps, recur_map, input_map, decay_param, decay_offset, mix_proj):
    residual = tokens
    for layer_index in range(LAYERS):
        residual = mixer_layer(residual, norm_gain[layer_index], value_proj[layer_index], gate_proj[layer_index], conv_taps[layer_index], recur_map[layer_index], input_map[layer_index], decay_param[layer_index], decay_offset[layer_index], mix_proj[layer_index])
    return residual
```

```python
import functools

import jax
import jax.numpy as jnp
from jax import lax
from jax.experimental import pallas as pl
from jax.experimental.pallas import tpu as pltpu
from jax.sharding import PartitionSpec as P

LAYERS = 2
EPS = 1e-06
RATE_SCALE = 8.0
LANES = 128
F32 = jnp.float32
BF16 = jnp.bfloat16


def log1p_series(u):
    z = u / (2.0 + u)
    zz = z * z
    acc = jnp.full_like(zz, 1.0 / 17.0)
    for n in (15, 13, 11, 9, 7, 5, 3, 1):
        acc = acc * zz + 1.0 / n
    return 2.0 * z * acc


def softplus(v):
    return jnp.maximum(v, 0.0) + log1p_series(jnp.exp(-jnp.abs(v)))


def minus_expm1(y, ey):
    acc = jnp.full_like(y, 1.0 / 8.0)
    for n in (7, 6, 5, 4, 3, 2):
        acc = (acc * y + 1.0) * (1.0 / n)
    small = -(acc * y + 1.0) * y
    return jnp.where(y > -0.4, small, 1.0 - ey)


def sigmoid(v):
    return 1.0 / (1.0 + jnp.exp(-v))


def half_turn(v):
    return pltpu.roll(v, LANES // 2, 1)


def twice(row):
    return jnp.concatenate([row, row], axis=1)


def scan_rows(a, b):
    rows = a.shape[0]
    at = lax.broadcasted_iota(jnp.int32, a.shape, 0)
    d = 1
    while d < rows:
        if d < 8:
            kept = at >= d
            b = b + a * jnp.where(kept, pltpu.roll(b, d, 0), 0.0)
            a = a * jnp.where(kept, pltpu.roll(a, d, 0), 1.0)
        else:
            b = jnp.concatenate([b[:d], b[d:] + a[d:] * b[:-d]], axis=0)
            a = jnp.concatenate([a[:d], a[d:] * a[:-d]], axis=0)
        d *= 2
    return a, b


def kernel(
    sp_n,
    tp_n,
    tok_ref,
    gain_ref,
    value_ref,
    gate_ref,
    taps_ref,
    recur_ref,
    input_ref,
    param_ref,
    offset_ref,
    mix_ref,
    out_ref,
    xbuf,
    bbuf,
    wbuf,
    bd,
    gw,
    offp,
    vpad,
    halo_out,
    halo_in,
    carry,
    zs,
    zr,
    xs,
    xr,
    hs,
    hr,
    cs,
    cr,
):
    sp = lax.axis_index("sp")
    tp = lax.axis_index("tp")
    core = lax.rem(tp, 2)
    chip = tp // 2
    partner = tp + 1 - 2 * core
    chips = tp_n // 2
    rounds = sp_n // 4
    tok = tok_ref.shape[0]
    half = tok // 2
    ch = value_ref.shape[1]

    def on_sp(step):
        return lax.rem(sp + (step + sp_n), sp_n)

    def on_tp(step):
        return 2 * lax.rem(chip + (step + chips), chips) + core

    offsets = [chips // 2]
    for k in range(1, chips // 2 + 1):
        offsets += [o for o in (chips // 2 + k, chips // 2 - k) if 0 < o < chips]

    barrier = pltpu.get_barrier_semaphore()
    z_steps = (1, 2, -1, -2) if sp_n > 4 else (1, 2, -1)
    for step in z_steps:
        pl.semaphore_signal(barrier, inc=1, device_id={"sp": on_sp(step)})
    for off in offsets:
        pl.semaphore_signal(barrier, inc=1, device_id={"tp": on_tp(off)})
    pl.semaphore_signal(barrier, inc=1, device_id={"tp": partner})
    peers = len(z_steps) + len(offsets) + 1

    def cols(j):
        return pl.ds(pl.multiple_of(j * LANES, LANES), LANES)

    def w_slot(layer):
        return lambda j: wbuf.at[layer, :, cols(j)]

    def m_slot(layer):
        return lambda j: bd.at[layer, pl.ds(pl.multiple_of(j * LANES, LANES), ch), pl.ds(0, LANES)]

    sends = []

    def put(src, dst, send, recv, **where):
        copy = pltpu.make_async_remote_copy(
            src_ref=src,
            dst_ref=dst,
            send_sem=send,
            recv_sem=recv,
            device_id=where,
            device_id_type=pl.DeviceIdType.MESH,
        )
        copy.start()
        sends.append(copy)

    def arrived(slot, sem):
        pltpu.make_async_copy(slot, slot, sem).wait()

    def z_round(stream, slot, k):
        moves = [(1, 0, -2 * k), (2, 1, -2 * k), (-1, 2, 2 * k)]
        if k < rounds - 1:
            moves.append((-2, 3, 2 * k))
        if k > 0:
            for block in (on_sp(-2 * k), on_sp(2 * k)):
                arrived(slot(block), zr.at[stream, block])
        for step, lane, off in moves:
            block = on_sp(off)
            put(slot(block), slot(block), zs.at[stream, k, lane], zr.at[stream, block], sp=on_sp(step))

    def z_finish(stream, slot):
        for k in range(rounds):
            for off in (-2 * k - 1, 2 * k + 1):
                arrived(slot(on_sp(off)), zr.at[stream, on_sp(off)])
        far = on_sp(-2 * rounds)
        arrived(slot(far), zr.at[stream, far])

    def x_start(g, slot):
        own = slot(tp)
        for n, off in enumerate(offsets):
            put(own, own, xs.at[g, n], xr.at[g, tp], tp=on_tp(off))
        put(own, own, xs.at[g, len(offsets)], xr.at[g, tp], tp=partner)

    def x_pass(g, slot, which):
        for n in which:
            block = on_tp(-offsets[n])
            arrived(slot(block), xr.at[g, block])
            put(slot(block), slot(block), xs.at[g, len(offsets) + 1 + n], xr.at[g, block], tp=partner)

    def x_finish(g, slot):
        for k in range(chips):
            block = 2 * k + (1 - core)
            arrived(slot(block), xr.at[g, block])

    lo8 = lax.broadcasted_iota(jnp.int32, (8, LANES), 1) < LANES // 2
    lo1 = lax.broadcasted_iota(jnp.int32, (1, LANES), 1) < LANES // 2
    lo = lax.broadcasted_iota(jnp.int32, (half, LANES), 1) < LANES // 2

    def own_weights(layer):
        gain = gain_ref[pl.ds(layer, 1), cols(sp)]
        both = jnp.concatenate([value_ref[layer], gate_ref[layer]], axis=0)
        wbuf[layer, :, cols(sp)] = (both.astype(F32) * gain).astype(BF16)

    def own_mix(layer):
        bd[layer, pl.ds(pl.multiple_of(sp * LANES, LANES), ch), 0:LANES] = mix_ref[layer]

    x_slot = lambda layer: (lambda j: xbuf.at[layer, :, cols(j)])
    b_slot = lambda layer: (lambda j: bbuf.at[layer, :, cols(j)])

    own_weights(0)
    xbuf[0, :, cols(tp)] = tok_ref[...]
    own_mix(0)
    own_weights(1)
    own_mix(1)

    pl.semaphore_wait(barrier, peers)
    z_round(0, w_slot(0), 0)
    x_start(0, x_slot(0))

    rates = []
    for layer in range(LAYERS):
        z64 = jnp.zeros((ch, LANES // 2), BF16)
        r, i = recur_ref[layer, 0], input_ref[layer, 0]
        gw[layer] = jnp.concatenate(
            [
                jnp.concatenate([r, z64, i, z64], axis=1),
                jnp.concatenate([z64, r, z64, i], axis=1),
            ],
            axis=0,
        )
        stacked = jnp.concatenate([offset_ref[layer, :, 0:half], offset_ref[layer, :, half:]], axis=0)
        offp[layer] = stacked.T
        rates.append(twice(-RATE_SCALE * softplus(-param_ref[pl.ds(layer, 1), :])))
        for j in range(tp_n):
            bd[layer, j * LANES : j * LANES + ch, LANES:] = jnp.zeros((ch, LANES), BF16)
            bd[layer, j * LANES + ch : (j + 1) * LANES, 0:LANES] = jnp.zeros((LANES - ch, LANES), BF16)

    def project(layer):
        total = jnp.zeros((tok, LANES), F32)
        for j in range(tp_n):
            block = xbuf[layer, :, j * LANES : (j + 1) * LANES].astype(F32)
            total = total + block * block
        scale = lax.rsqrt(jnp.sum(total, axis=1, keepdims=True) / (tp_n * LANES) + EPS)
        product = lax.dot_general(
            xbuf[layer], wbuf[layer], (((1,), (1,)), ((), ())), preferred_element_type=F32
        )
        return product * scale

    def halo_copy(layer):
        return pltpu.make_async_remote_copy(
            src_ref=halo_out.at[layer],
            dst_ref=halo_in.at[layer],
            send_sem=hs.at[layer],
            recv_sem=hr.at[layer],
            device_id={"sp": on_sp(1)},
            device_id_type=pl.DeviceIdType.MESH,
        )

    def carry_copy(layer, k):
        return pltpu.make_async_remote_copy(
            src_ref=carry.at[layer, sp],
            dst_ref=carry.at[layer, sp],
            send_sem=cs.at[layer, k],
            recv_sem=cr.at[layer, sp],
            device_id={"sp": k},
            device_id_type=pl.DeviceIdType.MESH,
        )

    def recurrence(layer, beside_carry):
        rows = project(layer)
        halo_out[layer] = rows[tok - 8 :]

        @pl.when(sp < sp_n - 1)
        def _():
            halo_copy(layer).start()

        top, bottom = rows[:half], rows[half:]
        values = jnp.where(lo, top, half_turn(bottom))
        gates = jnp.where(lo, half_turn(top), bottom)
        gated = gates * sigmoid(gates)
        vpad[8:, :] = values
        within = half_turn(top[half - 8 :])

        @pl.when(sp > 0)
        def _():
            halo_copy(layer).wait_recv()

        @pl.when(sp == 0)
        def _():
            halo_in[layer] = jnp.zeros((8, LANES), F32)

        vpad[0:8, :] = jnp.where(lo8, halo_in[layer], within)
        smoothed = jnp.zeros((half, LANES), F32)
        taps_n = taps_ref.shape[1]
        for k in range(taps_n):
            tap = twice(taps_ref[layer, k : k + 1, :])
            first = 8 - (taps_n - 1) + k
            smoothed = smoothed + tap * vpad[first : first + half, :]
        maps = jnp.dot(smoothed.astype(BF16), gw[layer], preferred_element_type=F32)
        recur = sigmoid(maps[:, :LANES])
        inputs = sigmoid(maps[:, LANES:])
        log_decay = recur * rates[layer] + offp[layer]
        decay = jnp.exp(log_decay)
        driving = jnp.sqrt(minus_expm1(2.0 * log_decay, decay * decay)) * inputs * smoothed
        a, b = scan_rows(decay, driving)
        a_end, b_end = a[half - 1 :], b[half - 1 :]
        a_turn, b_turn = half_turn(a_end), half_turn(b_end)
        whole = jnp.where(lo1, a_end * a_turn, half_turn(a_turn * b_end + b_turn))
        carry[layer, sp] = whole

        def send(k, _):
            carry_copy(layer, k).start()
            return 0

        lax.fori_loop(sp + 1, sp_n, send, 0)
        beside_carry()
        a, b = a * gated, b * gated

        def fold(k, state):
            arrived(carry.at[layer, k], cr.at[layer, k])
            row = carry[layer, k]
            return half_turn(row) + row * state

        state = lax.fori_loop(0, sp, fold, jnp.zeros((1, LANES), F32))
        state = jnp.where(lo1, state, half_turn(b_end + a_end * state))
        bbuf[layer, :, cols(tp)] = (b + a * state).astype(BF16)

    def mixed(layer):
        for j in range(tp_n):
            bd[layer, j * LANES + ch : (j + 1) * LANES, LANES:] = bd[layer, j * LANES : j * LANES + ch, 0:LANES]
        out = jnp.dot(bbuf[layer], bd[layer], preferred_element_type=F32)
        own = xbuf[layer, :, cols(tp)].astype(F32)
        both = jnp.concatenate([out[:, :LANES], out[:, LANES:]], axis=0)
        return (own + both).astype(BF16)

    def thirds(parts):
        n = len(offsets)
        return [range(n * p // parts, n * (p + 1) // parts) for p in range(parts)]

    pieces = thirds(rounds)
    for k in range(rounds):
        if k > 0:
            z_round(0, w_slot(0), k)
        if k == rounds - 1:
            z_round(1, m_slot(0), 0)
        x_pass(0, x_slot(0), pieces[k])
    x_finish(0, x_slot(0))
    z_finish(0, w_slot(0))

    def more(stream, slot, first, last):
        for k in range(first, min(last, rounds)):
            z_round(stream, slot, k)

    recurrence(0, lambda: more(1, m_slot(0), 1, 2))
    x_start(1, b_slot(0))
    more(1, m_slot(0), 2, 3)
    more(2, w_slot(1), 0, 1)
    a, b = thirds(2)
    x_pass(1, b_slot(0), a)
    more(1, m_slot(0), 3, rounds)
    more(2, w_slot(1), 1, 2)
    x_pass(1, b_slot(0), b)
    x_finish(1, b_slot(0))
    z_finish(1, m_slot(0))
    xbuf[1, :, cols(tp)] = mixed(0)
    x_start(2, x_slot(1))
    more(2, w_slot(1), 2, 3)
    more(3, m_slot(1), 0, 1)
    x_pass(2, x_slot(1), a)
    more(2, w_slot(1), 3, rounds)
    more(3, m_slot(1), 1, 2)
    x_pass(2, x_slot(1), b)
    x_finish(2, x_slot(1))
    z_finish(2, w_slot(1))
    recurrence(1, lambda: more(3, m_slot(1), 2, 3))
    x_start(3, b_slot(1))
    more(3, m_slot(1), 3, rounds)
    x_pass(3, b_slot(1), range(len(offsets)))
    x_finish(3, b_slot(1))
    z_finish(3, m_slot(1))
    out_ref[...] = mixed(1)

    for copy in sends:
        copy.wait_send()
    for layer in range(LAYERS):

        @pl.when(sp < sp_n - 1)
        def _():
            halo_copy(layer).wait_send()

        def sent(k, _):
            carry_copy(layer, k).wait_send()
            return 0

        lax.fori_loop(sp + 1, sp_n, sent, 0)


def solution(mesh):
    sp_n, tp_n = mesh.shape["sp"], mesh.shape["tp"]

    def local(*arrays):
        tok, wide = arrays[0].shape
        ch = arrays[2].shape[1]
        half = tok // 2
        full = tp_n * wide
        vmem = pl.BlockSpec(memory_space=pltpu.VMEM)
        dma = pltpu.SemaphoreType.DMA
        sent = 2 * (tp_n // 2)
        return pl.pallas_call(
            functools.partial(kernel, sp_n, tp_n),
            out_shape=jax.ShapeDtypeStruct((tok, wide), BF16),
            in_specs=[vmem] * len(arrays),
            out_specs=vmem,
            scratch_shapes=[
                pltpu.VMEM((LAYERS, tok, full), BF16),
                pltpu.VMEM((LAYERS, half, tp_n * LANES), BF16),
                pltpu.VMEM((LAYERS, 2 * ch, full), BF16),
                pltpu.VMEM((LAYERS, tp_n * LANES, 2 * LANES), BF16),
                pltpu.VMEM((LAYERS, 2 * ch, 2 * LANES), BF16),
                pltpu.VMEM((LAYERS, half, LANES), F32),
                pltpu.VMEM((half + 8, LANES), F32),
                pltpu.VMEM((LAYERS, 8, LANES), F32),
                pltpu.VMEM((LAYERS, 8, LANES), F32),
                pltpu.VMEM((LAYERS, sp_n, 1, LANES), F32),
                dma((2 * LAYERS, sp_n // 4, 4)),
                dma((2 * LAYERS, sp_n)),
                dma((2 * LAYERS, sent)),
                dma((2 * LAYERS, tp_n)),
                dma((LAYERS,)),
                dma((LAYERS,)),
                dma((LAYERS, sp_n)),
                dma((LAYERS, sp_n)),
            ],
            compiler_params=pltpu.CompilerParams(collective_id=0, has_side_effects=True),
        )(*arrays)

    in_specs = (
        P(("grp", "sp"), "tp"),
        P(),
        P(None, "tp", "sp"),
        P(None, "tp", "sp"),
        P(None, None, "tp"),
        P(None, "tp", None, None),
        P(None, "tp", None, None),
        P(None, "tp"),
        P(None, "tp", "sp"),
        P(None, "sp", "tp"),
    )
    out_specs = P(("grp", "sp"), "tp")
    return jax.shard_map(local, mesh=mesh, in_specs=in_specs, out_specs=out_specs, check_vma=False)
```

```python
import functools

import jax
import jax.numpy as jnp
from jax import lax
from jax.experimental import pallas as pl
from jax.experimental.pallas import tpu as pltpu
from jax.sharding import PartitionSpec as P

LAYERS = 2
EPS = 1e-06
RATE_SCALE = 8.0
LANES = 128
F32 = jnp.float32
BF16 = jnp.bfloat16


def log1p_series(u):
    z = u / (2.0 + u)
    zz = z * z
    acc = jnp.full_like(zz, 1.0 / 17.0)
    for n in (15, 13, 11, 9, 7, 5, 3, 1):
        acc = acc * zz + 1.0 / n
    return 2.0 * z * acc


def softplus(v):
    return jnp.maximum(v, 0.0) + log1p_series(jnp.exp(-jnp.abs(v)))


def minus_expm1(y, ey):
    acc = jnp.full_like(y, 1.0 / 8.0)
    for n in (7, 6, 5, 4, 3, 2):
        acc = (acc * y + 1.0) * (1.0 / n)
    small = -(acc * y + 1.0) * y
    return jnp.where(y > -0.4, small, 1.0 - ey)


def sigmoid(v):
    return 1.0 / (1.0 + jnp.exp(-v))


def half_turn(v):
    return pltpu.roll(v, LANES // 2, 1)


def twice(row):
    return jnp.concatenate([row, row], axis=1)


def scan_rows(a, b):
    rows = a.shape[0]
    at = lax.broadcasted_iota(jnp.int32, a.shape, 0)
    d = 1
    while d < rows:
        if d < 8:
            kept = at >= d
            b = b + a * jnp.where(kept, pltpu.roll(b, d, 0), 0.0)
            a = a * jnp.where(kept, pltpu.roll(a, d, 0), 1.0)
        else:
            b = jnp.concatenate([b[:d], b[d:] + a[d:] * b[:-d]], axis=0)
            a = jnp.concatenate([a[:d], a[d:] * a[:-d]], axis=0)
        d *= 2
    return a, b


def kernel(sp_n, tp_n, *refs):
    (tok_hbm, gain_hbm, value_hbm, gate_hbm, taps_hbm, recur_hbm, input_hbm, param_hbm, offset_hbm, mix_hbm) = refs[:10]
    out_ref = refs[10]
    (gain_ref, value_ref, gate_ref, taps_ref, recur_ref, input_ref, param_ref, offset_ref, mix_ref) = refs[11:20]
    (xbuf, bbuf, wbuf, bd, gw, offp, vpad, squares, halo_out, halo_in, carry) = refs[20:31]
    (ls, zs, zr, xs, xr, hs, hr, cs, cr) = refs[31:]
    sp = lax.axis_index("sp")
    tp = lax.axis_index("tp")
    core = lax.rem(tp, 2)
    chip = tp // 2
    partner = tp + 1 - 2 * core
    chips = tp_n // 2
    stride = sp_n // 4
    hop = max(chips // 4, 1)
    tok = xbuf.shape[1]
    half = tok // 2
    ch = value_ref.shape[1]

    def on_sp(step):
        return lax.rem(sp + (step + sp_n), sp_n)

    def on_tp(step):
        return 2 * lax.rem(chip + (step + chips), chips) + core

    offsets = [chips // 2]
    for k in range(1, chips // 2 + 1):
        offsets += [o for o in (chips // 2 + k, chips // 2 - k) if 0 < o < chips]

    barrier = pltpu.get_barrier_semaphore()
    z_steps = [sign * step for step in range(stride, 0, -1) for sign in (1, -1)]
    for step in z_steps:
        pl.semaphore_signal(barrier, inc=1, device_id={"sp": on_sp(step)})
    for off in offsets:
        pl.semaphore_signal(barrier, inc=1, device_id={"tp": on_tp(off)})
    pl.semaphore_signal(barrier, inc=1, device_id={"tp": partner})
    peers = len(z_steps) + len(offsets) + 1

    def cols(j):
        return pl.ds(pl.multiple_of(j * LANES, LANES), LANES)

    local_copies = [
        pltpu.make_async_copy(src, dst, ls.at[n])
        for n, (src, dst) in enumerate(
            [
                (tok_hbm, xbuf.at[0, :, cols(tp)]),
                (gain_hbm, gain_ref),
                (value_hbm, value_ref),
                (gate_hbm, gate_ref),
                (mix_hbm, mix_ref),
                (taps_hbm, taps_ref),
                (recur_hbm, recur_ref),
                (input_hbm, input_ref),
                (param_hbm, param_ref),
                (offset_hbm, offset_ref),
            ]
        )
    ]
    for copy in local_copies:
        copy.start()

    def put(src, dst, send, recv, **where):
        pltpu.make_async_remote_copy(
            src_ref=src,
            dst_ref=dst,
            send_sem=send,
            recv_sem=recv,
            device_id=where,
            device_id_type=pl.DeviceIdType.MESH,
        ).start()

    def arrived(slot, sem):
        pltpu.make_async_copy(slot, slot, sem).wait()

    class Weights:
        def __init__(self, n, slot, many):
            self.n, self.slot, self.many = n, slot, many

        def send(self, block, step, relayed):
            n, slot = self.n, self.slot(block)
            lane = (0 if relayed > 0 else 1) if relayed else 2
            put(slot, slot, zs.at[n], zr.at[n, lane], sp=on_sp(step))

        def first(self):
            for step in z_steps:
                self.send(sp, step, step if abs(step) == stride else 0)

        def second(self):
            for sign, lane in ((1, 0), (-1, 1)):
                block = on_sp(-sign * stride)
                arrived(self.slot(block), zr.at[self.n, lane])
                for step in range(stride if sign > 0 else stride - 1, 0, -1):
                    self.send(block, sign * step, 0)

        def finish(self):
            arrived(self.many(sp_n - 3), zr.at[self.n, 2])

        def sent(self):
            arrived(self.many(sp_n - 1), zs.at[self.n])

    def w_rows(n, layer, first, count):
        return Weights(
            n,
            lambda j: wbuf.at[layer, first : first + count, cols(j)],
            lambda k: wbuf.at[layer, first : first + count, 0 : k * LANES],
        )

    def m_rows(n, layer):
        return Weights(
            n,
            lambda j: bd.at[layer, pl.ds(pl.multiple_of(j * LANES, LANES), ch), 0:LANES],
            lambda k: bd.at[layer, 0 : k * ch, 0:LANES],
        )

    w_value, w_gate, w_next = w_rows(0, 0, 0, ch), w_rows(1, 0, ch, ch), w_rows(2, 1, 0, 2 * ch)
    mixes = (m_rows(3, 0), m_rows(4, 1))

    class Tokens:
        def __init__(self, n, layer):
            self.n, self.layer = n, layer

        def slot(self, j, rows=None):
            return xbuf.at[self.layer, slice(0, tok) if rows is None else pl.ds(*rows), cols(j)]

        def put(self, lane, block, rows=None, **where):
            slot = self.slot(block, rows)
            put(slot, slot, xs.at[self.n], xr.at[self.n, lane], **where)

        def hand(self, block, lane):
            self.put(lane, block, tp=partner)

        def got(self, lane, block, rows=None):
            arrived(self.slot(block, rows), xr.at[self.n, lane])

        def first(self):
            for step in range(hop, 0, -1):
                self.put(2 + step, tp, tp=on_tp(step))
                if chips > 2:
                    self.put(2 + hop + step, tp, tp=on_tp(-step))
            self.hand(tp, 0)

        def second(self):
            if chips > 2:
                for sign in (1, -1):
                    block, at = on_tp(-sign * hop), 2 + (0 if sign > 0 else hop)
                    self.got(at + hop, block)
                    rows = (0 if sign > 0 else half, half)
                    self.put(3 + 2 * hop + (0 if sign > 0 else 1), block, rows, tp=on_tp(sign * hop))
                    for step in range(hop - 1, 0, -1):
                        self.put(4 + 2 * hop + (0 if sign > 0 else hop - 1) + step, block, tp=on_tp(sign * step))
                    self.hand(block, 0)
                    square(self.layer, block)
                for sign in (1, -1):
                    for step in range(1, hop):
                        block = on_tp(-sign * step)
                        self.got(2 + (0 if sign > 0 else hop) + step, block)
                        self.hand(block, 0)
                        square(self.layer, block)
            else:
                block = on_tp(1)
                self.got(2 + hop, block)
                self.hand(block, 0)
                square(self.layer, block)
            square(self.layer, tp)

        def third(self):
            if chips > 2:
                for sign in (1, -1):
                    for step in range(1, hop):
                        block = on_tp(-sign * (hop + step))
                        self.got(4 + 2 * hop + (0 if sign > 0 else hop - 1) + step, block)
                        self.hand(block, 1)
                        square(self.layer, block)
                block = on_tp(chips // 2)
                self.got(3 + 2 * hop, block, (0, half))
                self.got(4 + 2 * hop, block, (half, half))
                self.hand(block, 1)
                square(self.layer, block)

        def near(self):
            return 2 if chips == 2 else 1 + 2 * hop

        def finish(self):
            near = self.near()
            arrived(xbuf.at[self.layer, :, 0 : near * LANES], xr.at[self.n, 0])
            for step in range(-hop, hop + 1) if chips > 2 else (0, 1):
                square(self.layer, on_tp(step) + 1 - 2 * core)
            if chips > near:
                arrived(xbuf.at[self.layer, :, 0 : (chips - near) * LANES], xr.at[self.n, 1])
                for step in range(hop + 1, chips - hop):
                    square(self.layer, on_tp(step) + 1 - 2 * core)

        def sent(self):
            total = 2 * chips - 1
            arrived(xbuf.at[self.layer, :, 0 : total * LANES], xs.at[self.n])

    class Branches:
        def __init__(self, n, layer):
            self.n, self.layer = n, layer

        def put(self, lane, block, **where):
            slot = bbuf.at[self.layer, :, cols(block)]
            put(slot, slot, xs.at[self.n], xr.at[self.n, lane], **where)

        def first(self):
            for n, off in enumerate(offsets):
                self.put(1 + n, tp, tp=on_tp(off))
            self.put(0, tp, tp=partner)

        def second(self):
            for n, off in enumerate(offsets):
                block = on_tp(-off)
                arrived(bbuf.at[self.layer, :, cols(block)], xr.at[self.n, 1 + n])
                self.put(0, block, tp=partner)

        def finish(self):
            arrived(bbuf.at[self.layer, :, 0 : chips * LANES], xr.at[self.n, 0])

        def sent(self):
            arrived(bbuf.at[self.layer, :, 0 : (2 * chips - 1) * LANES], xs.at[self.n])

    lo8 = lax.broadcasted_iota(jnp.int32, (8, LANES), 1) < LANES // 2
    lo1 = lax.broadcasted_iota(jnp.int32, (1, LANES), 1) < LANES // 2

    def square(layer, block):
        wide = xbuf[layer, :, cols(block)].astype(F32)
        squares[...] += wide * wide

    def own_weights(layer):
        gain = gain_ref[pl.ds(layer, 1), cols(sp)]
        both = jnp.concatenate([value_ref[layer], gate_ref[layer]], axis=0)
        wbuf[layer, :, cols(sp)] = (both.astype(F32) * gain).astype(BF16)

    tokens = (Tokens(0, 0), Tokens(1, 1))
    branches = (Branches(2, 0), Branches(3, 1))

    for copy in local_copies[:4]:
        copy.wait()
    own_weights(0)
    pl.semaphore_wait(barrier, peers)
    w_value.first()
    tokens[0].first()
    w_gate.first()

    for copy in local_copies[4:]:
        copy.wait()
    own_weights(1)
    squares[...] = jnp.zeros((tok, LANES), F32)
    rates = []
    for layer in range(LAYERS):
        bd[layer, pl.ds(pl.multiple_of(sp * LANES, LANES), ch), 0:LANES] = mix_ref[layer]
        z64 = jnp.zeros((ch, LANES // 2), BF16)
        r, i = recur_ref[layer, 0], input_ref[layer, 0]
        gw[layer] = jnp.concatenate(
            [
                jnp.concatenate([r, z64, i, z64], axis=1),
                jnp.concatenate([z64, r, z64, i], axis=1),
            ],
            axis=0,
        )
        stacked = jnp.concatenate([offset_ref[layer, :, 0:half], offset_ref[layer, :, half:]], axis=0)
        offp[layer] = stacked.T
        rates.append(twice(-RATE_SCALE * softplus(-param_ref[pl.ds(layer, 1), :])))
        for j in range(tp_n):
            bd[layer, j * LANES : j * LANES + ch, LANES:] = jnp.zeros((ch, LANES), BF16)
            bd[layer, j * LANES + ch : (j + 1) * LANES, 0:LANES] = jnp.zeros((LANES - ch, LANES), BF16)

    def product(layer, rows, first):
        return lax.dot_general(
            xbuf[layer, rows, :],
            wbuf[layer, first : first + ch, :],
            (((1,), (1,)), ((), ())),
            preferred_element_type=F32,
        )

    def halo_copy(layer):
        return pltpu.make_async_remote_copy(
            src_ref=halo_out.at[layer],
            dst_ref=halo_in.at[layer],
            send_sem=hs.at[layer],
            recv_sem=hr.at[layer],
            device_id={"sp": on_sp(1)},
            device_id_type=pl.DeviceIdType.MESH,
        )

    def carry_copy(layer, k):
        return pltpu.make_async_remote_copy(
            src_ref=carry.at[layer, sp],
            dst_ref=carry.at[layer, sp],
            send_sem=cs.at[k],
            recv_sem=cr.at[layer, sp],
            device_id={"sp": k},
            device_id_type=pl.DeviceIdType.MESH,
        )

    def carries_sent(layer):
        def sent(k, _):
            carry_copy(layer, k).wait_send()
            return 0

        lax.fori_loop(sp + 1, sp_n, sent, 0)

    def elements(layer, first, count):
        smoothed = jnp.zeros((count, LANES), F32)
        taps_n = taps_ref.shape[1]
        for k in range(taps_n):
            tap = twice(taps_ref[layer, k : k + 1, :])
            at = 8 + first - (taps_n - 1) + k
            smoothed = smoothed + tap * vpad[at : at + count, :]
        maps = jnp.dot(smoothed.astype(BF16), gw[layer], preferred_element_type=F32)
        recur = sigmoid(maps[:, :LANES])
        inputs = sigmoid(maps[:, LANES:])
        log_decay = recur * rates[layer] + offp[layer, first : first + count, :]
        decay = jnp.exp(log_decay)
        driving = jnp.sqrt(minus_expm1(2.0 * log_decay, decay * decay)) * inputs * smoothed
        return scan_rows(decay, driving)

    def recurrence(layer, before_gates, after_carry):
        scale = lax.rsqrt(jnp.sum(squares[...], axis=1, keepdims=True) / (tp_n * LANES) + EPS)
        bottom = product(layer, slice(half, tok), 0) * scale[half:]
        halo_out[layer] = jnp.concatenate([bottom[half - 8 :], jnp.zeros((8, LANES - ch), F32)], axis=1)

        @pl.when(sp < sp_n - 1)
        def _():
            halo_copy(layer).start()

        top = product(layer, slice(0, half), 0) * scale[:half]
        values = jnp.concatenate([top, bottom], axis=1)
        vpad[8:, :] = values
        within = half_turn(values[half - 8 :])
        a, b = elements(layer, 8, half - 8)

        @pl.when(sp > 0)
        def _():
            halo_copy(layer).wait_recv()

        @pl.when(sp == 0)
        def _():
            halo_in[layer] = jnp.zeros((8, LANES), F32)

        vpad[0:8, :] = jnp.where(lo8, halo_in[layer], within)
        a8, b8 = elements(layer, 0, 8)
        b = b + a * b8[7:]
        a = a * a8[7:]
        a = jnp.concatenate([a8, a], axis=0)
        b = jnp.concatenate([b8, b], axis=0)
        a_end, b_end = a[half - 1 :], b[half - 1 :]
        a_turn, b_turn = half_turn(a_end), half_turn(b_end)
        whole = jnp.where(lo1, a_end * a_turn, half_turn(a_turn * b_end + b_turn))
        carry[layer, sp] = whole

        def send(k, _):
            carry_copy(layer, k).start()
            return 0

        lax.fori_loop(sp + 1, sp_n, send, 0)
        before_gates()
        gates = jnp.concatenate(
            [product(layer, slice(0, half), ch) * scale[:half], product(layer, slice(half, tok), ch) * scale[half:]],
            axis=1,
        )
        gated = gates * sigmoid(gates)
        a, b = a * gated, b * gated
        after_carry()

        def fold(k, state):
            arrived(carry.at[layer, k], cr.at[layer, k])
            row = carry[layer, k]
            return half_turn(row) + row * state

        state = lax.fori_loop(0, sp, fold, jnp.zeros((1, LANES), F32))
        state = jnp.where(lo1, state, half_turn(b_end + a_end * state))
        bbuf[layer, :, cols(tp)] = (b + a * state).astype(BF16)

    def second_place(layer):
        for j in range(tp_n):
            bd[layer, j * LANES + ch : (j + 1) * LANES, LANES:] = bd[layer, j * LANES : j * LANES + ch, 0:LANES]

    def mixed(layer):
        out = jnp.dot(bbuf[layer], bd[layer], preferred_element_type=F32)
        own = xbuf[layer, :, cols(tp)].astype(F32)
        both = jnp.concatenate([out[:, :LANES], out[:, LANES:]], axis=0)
        return (own + both).astype(BF16)

    tokens[0].second()
    w_value.second()
    w_gate.second()
    tokens[0].third()
    tokens[0].finish()
    w_value.finish()

    def gates_here():
        mixes[0].first()
        w_gate.finish()

    recurrence(0, gates_here, lambda: None)
    branches[0].first()
    mixes[0].second()
    w_next.first()
    squares[...] = jnp.zeros((tok, LANES), F32)
    branches[0].second()
    mixes[0].finish()
    second_place(0)
    branches[0].finish()
    xbuf[1, :, cols(tp)] = mixed(0)
    tokens[1].first()
    w_next.second()
    mixes[1].first()
    tokens[1].second()
    tokens[1].third()
    tokens[1].finish()
    w_next.finish()
    carries_sent(0)
    recurrence(1, lambda: None, mixes[1].second)
    branches[1].first()
    mixes[1].finish()
    second_place(1)
    branches[1].second()
    branches[1].finish()
    out_ref[...] = mixed(1)

    for weights in (w_value, w_gate, w_next, *mixes):
        weights.sent()
    for gather in (*tokens, *branches):
        gather.sent()
    carries_sent(1)
    for layer in range(LAYERS):

        @pl.when(sp < sp_n - 1)
        def _():
            halo_copy(layer).wait_send()


def solution(mesh):
    sp_n, tp_n = mesh.shape["sp"], mesh.shape["tp"]

    def local(*arrays):
        tok, wide = arrays[0].shape
        ch = arrays[2].shape[1]
        half = tok // 2
        full = tp_n * wide
        chips = tp_n // 2
        dma = pltpu.SemaphoreType.DMA
        return pl.pallas_call(
            functools.partial(kernel, sp_n, tp_n),
            out_shape=jax.ShapeDtypeStruct((tok, wide), BF16),
            in_specs=[pl.BlockSpec(memory_space=pl.ANY)] * len(arrays),
            out_specs=pl.BlockSpec(memory_space=pltpu.VMEM),
            scratch_shapes=[
                *(pltpu.VMEM(a.shape, a.dtype) for a in (*arrays[1:4], *arrays[4:])),
                pltpu.VMEM((LAYERS, tok, full), BF16),
                pltpu.VMEM((LAYERS, half, tp_n * LANES), BF16),
                pltpu.VMEM((LAYERS, 2 * ch, full), BF16),
                pltpu.VMEM((LAYERS, tp_n * LANES, 2 * LANES), BF16),
                pltpu.VMEM((LAYERS, 2 * ch, 2 * LANES), BF16),
                pltpu.VMEM((LAYERS, half, LANES), F32),
                pltpu.VMEM((half + 8, LANES), F32),
                pltpu.VMEM((tok, LANES), F32),
                pltpu.VMEM((LAYERS, 8, LANES), F32),
                pltpu.VMEM((LAYERS, 8, LANES), F32),
                pltpu.VMEM((LAYERS, sp_n, 1, LANES), F32),
                dma((len(arrays),)),
                dma((5,)),
                dma((5, 3)),
                dma((2 * LAYERS,)),
                dma((2 * LAYERS, max(chips + 3, 10))),
                dma((LAYERS,)),
                dma((LAYERS,)),
                dma((sp_n,)),
                dma((LAYERS, sp_n)),
            ],
            compiler_params=pltpu.CompilerParams(collective_id=0, has_side_effects=True),
        )(*arrays)

    in_specs = (
        P(("grp", "sp"), "tp"),
        P(),
        P(None, "tp", "sp"),
        P(None, "tp", "sp"),
        P(None, None, "tp"),
        P(None, "tp", None, None),
        P(None, "tp", None, None),
        P(None, "tp"),
        P(None, "tp", "sp"),
        P(None, "sp", "tp"),
    )
    out_specs = P(("grp", "sp"), "tp")
    return jax.shard_map(local, mesh=mesh, in_specs=in_specs, out_specs=out_specs, check_vma=False)
```
